32 devices in a mesh: fs: 16 (over z, y, x), tp: 2 (over core).
Axes of the slice: x: 2, y: 2, z: 4, core: 2. Of those that a mesh axis runs over, the one named last changes fastest.
Arguments:
- tokens: bfloat16 [2048, 2048], P('fs'), may hold values from -6 to 6
- norm_gain: float32 [2048], replicated, may hold values from 0.1 to 1.9
- w_query: bfloat16 [2048, 1024], P('fs', 'tp'), may hold values from -0.125 to 0.125
- w_key: bfloat16 [2048, 1024], P('fs', 'tp'), may hold values from -0.125 to 0.125
- w_value: bfloat16 [2048, 2048], P('fs', 'tp'), may hold values from -0.125 to 0.125
- w_gate: bfloat16 [2048, 2048], P('fs', 'tp'), may hold values from -0.125 to 0.125
- mixer_gain: float32 [2048], P('tp'), may hold values from 0.1 to 1.9
- w_out: bfloat16 [2048, 2048], P('tp', 'fs'), may hold values from -0.125 to 0.125
- channel_gain: float32 [2048], replicated, may hold values from 0.1 to 1.9
- w_left: bfloat16 [2048, 3072], P('fs', 'tp'), may hold values from -0.125 to 0.125
- w_right: bfloat16 [2048, 3072], P('fs', 'tp'), may hold values from -0.125 to 0.125
- taps_left: float32 [3, 3072], P(None, 'tp'), may hold values from -3.5 to 3.5
- taps_right: float32 [3, 3072], P(None, 'tp'), may hold values from -3.5 to 3.5
- w_down: bfloat16 [3072, 2048], P('tp', 'fs'), may hold values from -0.109375 to 0.109375
Outputs:
- layer_out: bfloat16 [2048, 2048], P('fs')
The draws below stay inside these ranges and needn't reach their ends.
All inputs are finite; a program needn't handle non-finite values.
Results may differ from the reference program's by a relative error of at most 0.018.
Values may be sent and summed in bfloat16 or wider, within the bound.
A program may use at most 64 MiB of HBM per device.

```python
import jax
import jax.numpy as jnp
from jax import lax

D = 2048
HEADS = 8
DK = 128
DV = 256
FF = 3072
BLOCK = 128
SEQ_LEN = 128
QW = 1024
VW = 2048
TOKENS = 2048
N_TP = 2


def shard_levels(key, shape, pieces, least, top_value):
    level = 1.0
    for axis_at, shards_of in pieces:
        heights = jax.random.uniform(jax.random.fold_in(jax.random.fold_in(key, 6), axis_at), (shards_of,), jnp.float32, least / len(pieces), top_value / len(pieces))
        level = level * jnp.repeat(jnp.exp(heights), shape[axis_at] // shards_of).reshape((-1,) + (1,) * (len(shape) - 1 - axis_at))
    return level


def normal_values(own_key, dims, spread, most, shards=(), held_as=jnp.bfloat16):
    level = shard_levels(own_key, dims, shards, -0.22, 0.18) if shards else 1.0
    drawn = jax.random.normal(own_key, dims, jnp.float32) * spread * level
    return jnp.minimum(jnp.maximum(drawn, -most), most).astype(held_as)


def setup_inputs(seed: int = 0) -> dict:
    keys = jax.random.split(jax.random.key(seed), 15)
    tokens = normal_values(keys[0], (TOKENS, D), 1.0, 6.0, ((0, 16),))
    norm_gain = jnp.clip(1.0 + 0.18 * jax.random.normal(keys[1], (D,), jnp.float32), 0.1, 1.9)
    w_query = normal_values(keys[2], (D, QW), D ** -0.5, 0.125, ((0, 16), (1, 2)))
    w_key = normal_values(keys[3], (D, QW), D ** -0.5, 0.125, ((0, 16), (1, 2)))
    w_value = normal_values(keys[4], (D, VW), D ** -0.5, 0.125, ((0, 16), (1, 2)))
    w_gate = normal_values(keys[5], (D, VW), D ** -0.5, 0.125, ((0, 16), (1, 2)))
    mixer_gain = jnp.clip(1.0 + 0.18 * jax.random.normal(keys[6], (VW,), jnp.float32), 0.1, 1.9)
    w_out = normal_values(keys[7], (VW, D), VW ** -0.5, 0.125, ((0, 2), (1, 16)))
    channel_gain = jnp.clip(1.0 + 0.18 * jax.random.normal(keys[8], (D,), jnp.float32), 0.1, 1.9)
    w_left = normal_values(keys[9], (D, FF), D ** -0.5, 0.125, ((0, 16), (1, 2)))
    w_right = normal_values(keys[10], (D, FF), D ** -0.5, 0.125, ((0, 16), (1, 2)))
    taps_left = normal_values(keys[11], (3, FF), 3 ** -0.5, 3.5, ((1, 2),), jnp.float32)
    taps_right = normal_values(keys[12], (3, FF), 3 ** -0.5, 3.5, ((1, 2),), jnp.float32)
    w_down = normal_values(keys[13], (FF, D), FF ** -0.5, 0.109375, ((0, 2), (1, 16)))
    return dict(tokens=tokens, norm_gain=norm_gain, w_query=w_query, w_key=w_key, w_value=w_value, w_gate=w_gate, mixer_gain=mixer_gain, w_out=w_out, channel_gain=channel_gain, w_left=w_left, w_right=w_right, taps_left=taps_left, taps_right=taps_right, w_down=w_down)


highest = lax.Precision.HIGHEST

def scale_rows(rows_in, gain_vec):
    floats = rows_in.astype(jnp.float32)
    factor = lax.rsqrt(lax.optimization_barrier(jnp.mean(floats * floats, axis=-1, keepdims=True)) + 1e-06)
    return (floats * factor * gain_vec.astype(jnp.float32)).astype(jnp.bfloat16)

def decays(first_head, count):
    head_ids = first_head + jnp.arange(count, dtype=jnp.float32)
    return jnp.log(1.0 - 2.0 ** (-5.0 - head_ids))

def rotate(heads_in, positions):
    width = heads_in.shape[-1]
    half = width // 2
    freqs = 10000.0 ** (-jnp.arange(half, dtype=jnp.float32) / half)
    angles = positions[:, None] * freqs[None, :]
    cosine = jnp.cos(angles)
    sine = jnp.sin(angles)
    first_half = heads_in[..., :half]
    second_half = heads_in[..., half:]
    return jnp.concatenate([first_half * cosine - second_half * sine, first_half * sine + second_half * cosine], axis=-1)

def retention(queries, keys_in, values_in, log_gamma):
    head_count, length, key_width = queries.shape
    value_width = values_in.shape[-1]
    blocks = length // BLOCK
    queries = queries.reshape(head_count, blocks, BLOCK, key_width)
    keys_in = keys_in.reshape(head_count, blocks, BLOCK, key_width)
    values_in = values_in.reshape(head_count, blocks, BLOCK, value_width)
    offsets = jnp.arange(BLOCK, dtype=jnp.float32)
    distance = offsets[:, None] - offsets[None, :]
    weights = jnp.where(distance >= 0, jnp.exp(log_gamma[:, None, None] * jnp.maximum(distance, 0.0)), 0.0)
    scores = jnp.einsum('hbnd,hbmd->hbnm', queries, keys_in, precision=highest) * weights[:, None]
    inner = jnp.einsum('hbnm,hbme->hbne', scores, values_in, precision=highest)
    key_weight = jnp.exp(log_gamma[:, None] * (BLOCK - 1 - offsets)[None, :])
    contrib = jnp.einsum('hbjd,hbje->hbde', keys_in * key_weight[:, None, :, None], values_in, precision=highest)
    block_decay = jnp.exp(log_gamma * BLOCK)[:, None, None]

    def advance(state, contrib_block):
        return (state * block_decay + contrib_block, state)
    _, states = lax.scan(advance, jnp.zeros((head_count, key_width, value_width), jnp.float32), jnp.moveaxis(contrib, 1, 0))
    states = jnp.moveaxis(states, 0, 1)
    query_weight = jnp.exp(log_gamma[:, None] * (offsets + 1.0)[None, :])
    carried = jnp.einsum('hbnd,hbde->hbne', queries, states, precision=highest) * query_weight[:, None, :, None]
    return (inner + carried).reshape(head_count, length, value_width)

def head_norm(retained):
    return retained * lax.rsqrt(lax.optimization_barrier(jnp.mean(retained * retained, axis=-1, keepdims=True)) + 1e-06)

def causal_taps(values_in, taps):
    length = values_in.shape[-2]
    spacing = [(0, 0)] * (values_in.ndim - 2) + [(taps.shape[0] - 1, 0), (0, 0)]
    padded = jnp.pad(values_in.astype(jnp.float32), spacing)
    result = padded[..., 0:length, :] * taps[0]
    for tap_index in range(1, taps.shape[0]):
        result = result + padded[..., tap_index:tap_index + length, :] * taps[tap_index]
    return result

def group_sum(left, weight):
    span = left.shape[1] // N_TP
    running = jnp.zeros((left.shape[0], weight.shape[1]), jnp.float32)
    for group in range(N_TP):
        partial_sum = jnp.dot(left[:, group * span:(group + 1) * span], weight[group * span:(group + 1) * span], preferred_element_type=jnp.float32).astype(jnp.bfloat16)
        running = running + lax.optimization_barrier(partial_sum).astype(jnp.float32)
    return running

def reference(tokens, norm_gain, w_query, w_key, w_value, w_gate, mixer_gain, w_out, channel_gain, w_left, w_right, taps_left, taps_right, w_down):
    seq_count = tokens.shape[0] // SEQ_LEN
    normed = scale_rows(tokens, norm_gain)

    def project(source, weight):
        return jnp.dot(source, weight, preferred_element_type=jnp.float32).astype(jnp.bfloat16)
    queries = project(normed, w_query)
    keys_proj = project(normed, w_key)
    values_proj = project(normed, w_value)
    gates = project(normed, w_gate)
    positions = jnp.arange(SEQ_LEN, dtype=jnp.float32)
    log_gamma = decays(0.0, HEADS)

    def split_heads(rows_in, width):
        return rows_in.astype(jnp.float32).reshape(seq_count, SEQ_LEN, HEADS, width).transpose(0, 2, 1, 3)

    def one_sequence(triple):
        query_heads, key_heads, value_heads = triple
        return head_norm(retention(rotate(query_heads, positions), rotate(key_heads, positions), value_heads, log_gamma))
    retained = lax.map(one_sequence, (split_heads(queries, DK), split_heads(keys_proj, DK), split_heads(values_proj, DV)))
    retained = retained.transpose(0, 2, 1, 3).reshape(seq_count * SEQ_LEN, VW)
    hidden = (retained * mixer_gain * jax.nn.silu(gates.astype(jnp.float32))).astype(jnp.bfloat16)
    middle = (tokens.astype(jnp.float32) + group_sum(hidden, w_out)).astype(jnp.bfloat16)
    normed_mid = scale_rows(middle, channel_gain)
    left = project(normed_mid, w_left)
    right = project(normed_mid, w_right)

    def convolve(rows_in, taps):
        return causal_taps(rows_in.reshape(seq_count, SEQ_LEN, FF), taps).reshape(seq_count * SEQ_LEN, FF)
    gated = (jax.nn.silu(convolve(left, taps_left)) * convolve(right, taps_right)).astype(jnp.bfloat16)
    return (middle.astype(jnp.float32) + group_sum(gated, w_down)).astype(jnp.bfloat16)
```

```python
import functools

import jax
import jax.numpy as jnp
import numpy as np
from jax import lax
from jax.experimental import pallas as pl
from jax.experimental.pallas import tpu as pltpu
from jax.sharding import PartitionSpec as P

DK = 128
DV = 256
BLOCK = 128
MESH = pl.DeviceIdType.MESH


highest = lax.Precision.HIGHEST


def scale_rows(rows_in, gain_vec):
    floats = rows_in.astype(jnp.float32)
    factor = lax.rsqrt(jnp.mean(floats * floats, axis=-1, keepdims=True) + 1e-06)
    return (floats * factor * gain_vec).astype(jnp.bfloat16)


def decays(first_head, count):
    head_ids = first_head + jnp.arange(count, dtype=jnp.float32)
    return jnp.log(1.0 - 2.0 ** (-5.0 - head_ids))


def rotate(heads_in, positions):
    width = heads_in.shape[-1]
    half = width // 2
    freqs = 10000.0 ** (-jnp.arange(half, dtype=jnp.float32) / half)
    angles = positions[:, None] * freqs[None, :]
    cosine = jnp.cos(angles)
    sine = jnp.sin(angles)
    first_half = heads_in[..., :half]
    second_half = heads_in[..., half:]
    return jnp.concatenate(
        [first_half * cosine - second_half * sine, first_half * sine + second_half * cosine],
        axis=-1,
    )


def retention(queries, keys_in, values_in, log_gamma):
    head_count, length, key_width = queries.shape
    value_width = values_in.shape[-1]
    blocks = length // BLOCK
    queries = queries.reshape(head_count, blocks, BLOCK, key_width)
    keys_in = keys_in.reshape(head_count, blocks, BLOCK, key_width)
    values_in = values_in.reshape(head_count, blocks, BLOCK, value_width)
    offsets = jnp.arange(BLOCK, dtype=jnp.float32)
    distance = offsets[:, None] - offsets[None, :]
    weights = jnp.where(
        distance >= 0, jnp.exp(log_gamma[:, None, None] * jnp.maximum(distance, 0.0)), 0.0
    )
    scores = jnp.einsum("hbnd,hbmd->hbnm", queries, keys_in, precision=highest) * weights[:, None]
    inner = jnp.einsum("hbnm,hbme->hbne", scores, values_in, precision=highest)
    key_weight = jnp.exp(log_gamma[:, None] * (BLOCK - 1 - offsets)[None, :])
    contrib = jnp.einsum(
        "hbjd,hbje->hbde", keys_in * key_weight[:, None, :, None], values_in, precision=highest
    )
    block_decay = jnp.exp(log_gamma * BLOCK)[:, None, None]

    def advance(state, contrib_block):
        return (state * block_decay + contrib_block, state)

    _, states = lax.scan(
        advance,
        jnp.zeros((head_count, key_width, value_width), jnp.float32),
        jnp.moveaxis(contrib, 1, 0),
    )
    states = jnp.moveaxis(states, 0, 1)
    query_weight = jnp.exp(log_gamma[:, None] * (offsets + 1.0)[None, :])
    carried = (
        jnp.einsum("hbnd,hbde->hbne", queries, states, precision=highest)
        * query_weight[:, None, :, None]
    )
    return (inner + carried).reshape(head_count, length, value_width)


def head_norm(retained):
    return retained * lax.rsqrt(jnp.mean(retained * retained, axis=-1, keepdims=True) + 1e-06)


def causal_taps(values_in, taps):
    length = values_in.shape[-2]
    padded = jnp.pad(values_in.astype(jnp.float32), ((taps.shape[0] - 1, 0), (0, 0)))
    result = padded[0:length] * taps[0]
    for tap_index in range(1, taps.shape[0]):
        result = result + padded[tap_index : tap_index + length] * taps[tap_index]
    return result


def fold_single(source, weight_piece):
    return jnp.dot(source, weight_piece, preferred_element_type=jnp.float32)


def collect_single(source, weight):
    return fold_single(source, lax.all_gather(weight, "fs", axis=0, tiled=True))


def plain_body(
    tokens,
    norm_gain,
    w_query,
    w_key,
    w_value,
    w_gate,
    mixer_gain,
    w_out,
    channel_gain,
    w_left,
    w_right,
    taps_left,
    taps_right,
    w_down,
):
    length = tokens.shape[0]
    normed = scale_rows(tokens, norm_gain)
    queries = collect_single(normed, w_query)
    keys_proj = collect_single(normed, w_key)
    values_proj = collect_single(normed, w_value)
    gates = collect_single(normed, w_gate)
    queries = queries.astype(jnp.bfloat16)
    keys_proj = keys_proj.astype(jnp.bfloat16)
    values_proj = values_proj.astype(jnp.bfloat16)
    gates = gates.astype(jnp.bfloat16)
    heads_here = w_query.shape[1] // DK
    first_head = (lax.axis_index("tp") * heads_here).astype(jnp.float32)
    log_gamma = decays(first_head, heads_here)
    positions = jnp.arange(length, dtype=jnp.float32)

    def split_heads(rows_in, width):
        return rows_in.astype(jnp.float32).reshape(length, heads_here, width).transpose(1, 0, 2)

    retained = head_norm(
        retention(
            rotate(split_heads(queries, DK), positions),
            rotate(split_heads(keys_proj, DK), positions),
            split_heads(values_proj, DV),
            log_gamma,
        )
    )
    retained = retained.transpose(1, 0, 2).reshape(length, heads_here * DV)
    hidden = (retained * mixer_gain * jax.nn.silu(gates.astype(jnp.float32))).astype(jnp.bfloat16)
    rows_own = length // lax.axis_size("tp")
    first_row = lax.axis_index("tp") * rows_own
    out_whole = lax.all_gather(w_out, "fs", axis=1, tiled=True)
    mixer_total = lax.psum_scatter(
        jnp.dot(hidden, out_whole, preferred_element_type=jnp.float32).astype(jnp.bfloat16),
        "tp",
        scatter_dimension=0,
        tiled=True,
    ).astype(jnp.float32)
    residual = lax.dynamic_slice_in_dim(tokens, first_row, rows_own, 0)
    middle_own = (residual.astype(jnp.float32) + mixer_total).astype(jnp.bfloat16)
    middle = lax.all_gather(middle_own, "tp", axis=0, tiled=True)
    normed_mid = scale_rows(middle, channel_gain)
    left = collect_single(normed_mid, w_left)
    right = collect_single(normed_mid, w_right)
    left = left.astype(jnp.bfloat16)
    right = right.astype(jnp.bfloat16)
    gated = (jax.nn.silu(causal_taps(left, taps_left)) * causal_taps(right, taps_right)).astype(
        jnp.bfloat16
    )
    down_whole = lax.all_gather(w_down, "fs", axis=1, tiled=True)
    channel_part = jnp.dot(gated, down_whole, preferred_element_type=jnp.float32)
    channel_total = lax.psum(channel_part.astype(jnp.bfloat16), "tp").astype(jnp.float32)
    return (middle.astype(jnp.float32) + channel_total).astype(jnp.bfloat16)


def log_gammas(head_count):
    table = np.log(1.0 - 2.0 ** (-5.0 - np.arange(head_count, dtype=np.float64)))
    return np.repeat(table[:, None], BLOCK, axis=1).astype(np.float32)


def turning(length, width):
    half = width // 2
    freqs = np.float32(10000.0) ** (-np.arange(half, dtype=np.float32) / np.float32(half))
    angles = (np.arange(length, dtype=np.float32)[:, None] * freqs[None, :]).astype(np.float64)
    cosine, sine = np.cos(angles), np.sin(angles)
    return (
        np.concatenate([cosine, cosine], axis=1).astype(np.float32),
        np.concatenate([-sine, sine], axis=1).astype(np.float32),
    )


def silu(v):
    return v / (1.0 + jnp.exp(-v))


def normed_rows(floats, gain):
    factor = lax.rsqrt(jnp.mean(floats * floats, axis=-1, keepdims=True) + 1e-06)
    return (floats * factor * gain).astype(jnp.bfloat16)


def layer_kernel(
    n_fs,
    groups,
    tokens,
    norm_gain,
    wq,
    wk,
    wv,
    wg,
    mixer_gain,
    wo,
    channel_gain,
    wl,
    wr,
    taps_left,
    taps_right,
    wd,
    cos_t,
    sin_t,
    gammas,
    out,
    w1,
    wout,
    wlr,
    wdown,
    nt,
    nm,
    qkvg,
    hid,
    gated,
    part1,
    part2,
    xb1,
    xb2,
    sb1,
    sb2,
    rb1,
    rb2,
    mid,
    fin,
    fin_in,
    s1_send,
    s1_recv,
    self_sem,
    s2_send,
    s2_recv,
    a_send,
    a_recv,
    f_send,
    f_recv,
    x_send,
    x_recv,
    r_send,
    r_recv,
    o_send,
    o_recv,
):
    fs, tp = lax.axis_index("fs"), lax.axis_index("tp")
    planes = n_fs // groups
    z, q = fs // planes, lax.rem(fs, planes)
    other = 1 - tp
    length, width = tokens.shape
    own = length // 2
    kb = wq.shape[0]
    nb = wo.shape[1]
    cq, cv, cf = wq.shape[1] // groups, wv.shape[1] // groups, wl.shape[1] // groups

    def zpeer(step):
        return lax.rem(z + step, groups)

    def zback(step):
        return lax.rem(z + groups - step, groups)

    def zdev(target):
        return {"fs": target * planes + q, "tp": tp}

    def qdev(step):
        return {"fs": z * planes + lax.rem(q + step, planes), "tp": tp}

    partner = {"fs": fs, "tp": other}

    def lanes(index, size):
        return pl.ds(pl.multiple_of(index * size, 128), size)

    def rows(index, size):
        return pl.ds(pl.multiple_of(index * size, size), size)

    def region(cls, f):
        if cls == 0:
            return w1.at[rows(f, kb), :]
        if cls == 1:
            return wout.at[:, lanes(f, nb)]
        if cls == 2:
            return wlr.at[rows(f, kb), :]
        return wdown.at[:, lanes(f, nb)]

    pieces = (
        (0, lambda c: wq.at[:, lanes(c, cq)], lambda f: w1.at[rows(f, kb), pl.ds(0, cq)]),
        (0, lambda c: wk.at[:, lanes(c, cq)], lambda f: w1.at[rows(f, kb), pl.ds(cq, cq)]),
        (0, lambda c: wv.at[:, lanes(c, cv)], lambda f: w1.at[rows(f, kb), pl.ds(2 * cq, cv)]),
        (0, lambda c: wg.at[:, lanes(c, cv)], lambda f: w1.at[rows(f, kb), pl.ds(2 * cq + cv, cv)]),
        (1, lambda c: wo.at[rows(c, cv), :], lambda f: wout.at[:, lanes(f, nb)]),
        (2, lambda c: wl.at[:, lanes(c, cf)], lambda f: wlr.at[rows(f, kb), pl.ds(0, cf)]),
        (2, lambda c: wr.at[:, lanes(c, cf)], lambda f: wlr.at[rows(f, kb), pl.ds(cf, cf)]),
        (3, lambda c: wd.at[rows(c, cf), :], lambda f: wdown.at[:, lanes(f, nb)]),
    )

    barrier = pltpu.get_barrier_semaphore()
    for step in range(1, groups):
        pl.semaphore_signal(barrier, inc=1, device_id=zdev(zpeer(step)), device_id_type=MESH)
    for step in range(1, planes):
        pl.semaphore_signal(barrier, inc=1, device_id=qdev(step), device_id_type=MESH)
    pl.semaphore_signal(barrier, inc=1, device_id=partner, device_id_type=MESH)

    keeps = []
    for i, (cls, src, dst) in enumerate(pieces):
        keep = pltpu.make_async_copy(src(z), dst(fs), self_sem.at[i])
        keep.start()
        keeps.append(keep)

    def own_rows(seq, half):
        return pl.ds(pl.multiple_of(seq * length + half * own, own), own)

    my_half = pl.ds(pl.multiple_of(tp * own, own), own)
    nt[own_rows(z, tp), :] = normed_rows(tokens[my_half, :].astype(jnp.float32), norm_gain[...])
    pl.semaphore_wait(barrier, groups - 1 + planes - 1 + 1)

    def remote(src, dst, ssem, rsem, device):
        return pltpu.make_async_remote_copy(
            src_ref=src, dst_ref=dst, send_sem=ssem, recv_sem=rsem,
            device_id=device, device_id_type=MESH,
        )

    pending = []

    def go(copy):
        copy.start()
        pending.append(copy)

    def spread(buf, which):
        mine = buf.at[own_rows(z, tp), :]
        for step in range(1, groups):
            go(remote(mine, mine, a_send.at[which, step], a_recv.at[which, step], zdev(zpeer(step))))
        go(remote(mine, mine, f_send.at[which, 0], f_recv.at[which, 0], partner))

    def pass_on(buf, which):
        for step in range(1, groups):
            got = buf.at[own_rows(zback(step), tp), :]
            remote(got, got, a_send.at[which, step], a_recv.at[which, step], zdev(zpeer(step))).wait_recv()
            go(remote(got, got, f_send.at[which, step], f_recv.at[which, step], partner))

    def await_pass(buf, which):
        for step in range(groups):
            got = buf.at[own_rows(zback(step), other), :]
            remote(got, got, f_send.at[which, step], f_recv.at[which, step], partner).wait_recv()

    def first_leg(cls):
        for step in range(1, groups):
            for i, (c, src, dst) in enumerate(pieces):
                if c == cls:
                    target = zpeer(step)
                    go(remote(src(target), dst(fs), s1_send.at[i, step], s1_recv.at[i, step], zdev(target)))

    def second_leg(cls, step):
        f = zback(step) * planes + q
        for i, (c, src, dst) in enumerate(pieces):
            if c == cls:
                if step == 0:
                    keeps[i].wait()
                else:
                    remote(src(z), dst(f), s1_send.at[i, step], s1_recv.at[i, step], zdev(zpeer(step))).wait_recv()
        for hop in range(1, planes):
            go(remote(region(cls, f), region(cls, f), s2_send.at[cls, step, hop],
                      s2_recv.at[cls, step, hop], qdev(hop)))

    def await_leg(cls):
        for step in range(groups):
            for hop in range(1, planes):
                f = zback(step) * planes + lax.rem(q + planes - hop, planes)
                remote(region(cls, f), region(cls, f), s2_send.at[cls, step, hop],
                       s2_recv.at[cls, step, hop], qdev(hop)).wait_recv()

    spread(nt, 0)
    for cls in range(4):
        first_leg(cls)
    second_leg(0, 0)
    second_leg(2, 0)
    pass_on(nt, 0)
    for step in range(1, groups):
        second_leg(0, step)
    for step in range(groups):
        second_leg(1, step)
    await_pass(nt, 0)
    await_leg(0)

    head = tp * groups + z
    log_gamma = gammas[pl.ds(head, 1), :]
    distance = (
        lax.broadcasted_iota(jnp.int32, (length, length), 0)
        - lax.broadcasted_iota(jnp.int32, (length, length), 1)
    ).astype(jnp.float32)
    decay = jnp.where(distance >= 0, jnp.exp(log_gamma * jnp.maximum(distance, 0.0)), 0.0)
    chunk = 2 * length if (groups % 2 == 0) else length

    @pl.loop(0, groups * length // chunk)
    def _(at):
        span = rows(at, chunk)
        qkvg[span, :] = jnp.dot(
            nt[span, :], w1[...], preferred_element_type=jnp.float32
        ).astype(jnp.bfloat16)

    @pl.loop(0, groups)
    def _(at):
        span = rows(at, length)
        block = qkvg[span, :].astype(jnp.float32)

        def turn(x):
            return x * cos_t[...] + pltpu.roll(x, cq // 2, 1) * sin_t[...]

        rq = turn(block[:, :cq])
        rk = turn(block[:, cq : 2 * cq])
        scores = lax.dot_general(
            rq, rk, (((1,), (1,)), ((), ())), precision=highest, preferred_element_type=jnp.float32
        ) * decay
        kept = jnp.dot(
            scores, block[:, 2 * cq : 2 * cq + cv], precision=highest,
            preferred_element_type=jnp.float32,
        )
        kept = kept * lax.rsqrt(jnp.mean(kept * kept, axis=-1, keepdims=True) + 1e-06)
        gain = mixer_gain[:, lanes(z, cv)]
        hid[span, :] = (kept * gain * silu(block[:, 2 * cq + cv :])).astype(jnp.bfloat16)

    def total(left, weight, part, xb, sb, rb, which):
        for step in [*range(1, groups), 0]:
            g = zpeer(step)
            product = jnp.dot(
                left[rows(g, length), :], weight[...], preferred_element_type=jnp.float32
            ).astype(jnp.bfloat16)
            part[0, g] = product[:own]
            part[1, g] = product[own:]
            go(remote(part.at[other, g], xb.at[g], x_send.at[which, step], x_recv.at[which, step], partner))
        for step in [*range(1, groups), 0]:
            g = zpeer(step)
            remote(part.at[other, g], xb.at[g], x_send.at[which, step], x_recv.at[which, step], partner).wait_recv()
            pair = part[tp, g].astype(jnp.float32) + xb[g].astype(jnp.float32)
            if step:
                sb[step] = pair.astype(jnp.bfloat16)
                go(remote(sb.at[step], rb.at[step], r_send.at[which, step], r_recv.at[which, step], zdev(g)))
        return pair

    def gather_total(pair, sb, rb, which):
        for step in range(1, groups):
            remote(sb.at[step], rb.at[step], r_send.at[which, step], r_recv.at[which, step], zdev(zpeer(step))).wait_recv()
            pair = pair + rb[step].astype(jnp.float32)
        return pair

    await_leg(1)
    pair = total(hid, wout, part1, xb1, sb1, rb1, 0)
    mid[...] = pair
    for step in range(1, groups):
        second_leg(2, step)
    second_leg(3, 0)
    middle = (
        tokens[my_half, :].astype(jnp.float32) + gather_total(mid[...], sb1, rb1, 0)
    ).astype(jnp.bfloat16).astype(jnp.float32)
    mid[...] = middle
    nm[own_rows(z, tp), :] = normed_rows(middle, channel_gain[...])
    spread(nm, 1)
    for step in range(1, groups):
        second_leg(3, step)
    pass_on(nm, 1)
    await_pass(nm, 1)
    await_leg(2)

    @pl.loop(0, groups * length // chunk)
    def _(at):
        span = rows(at, chunk)
        both = jnp.dot(
            nm[span, :], wlr[...], preferred_element_type=jnp.float32
        ).astype(jnp.bfloat16).astype(jnp.float32)
        place = lax.rem(lax.broadcasted_iota(jnp.int32, (chunk, 1), 0), length)

        def convolve(x, taps):
            count = taps.shape[0]
            weights = taps[:, lanes(z, cf)]
            result = x * weights[count - 1 :, :]
            for back in range(1, count):
                moved = jnp.where(place >= back, pltpu.roll(x, back, 0), 0.0)
                result = result + moved * weights[count - 1 - back : count - back, :]
            return result

        gated[span, :] = (
            silu(convolve(both[:, :cf], taps_left)) * convolve(both[:, cf:], taps_right)
        ).astype(jnp.bfloat16)

    await_leg(3)
    pair = total(gated, wdown, part2, xb2, sb2, rb2, 1)
    fin[...] = (mid[...] + gather_total(pair, sb2, rb2, 1)).astype(jnp.bfloat16)
    last = remote(fin, fin_in, o_send, o_recv, partner)
    last.start()
    out[my_half, :] = fin[...]
    last.wait_recv()
    out[pl.ds(pl.multiple_of(other * own, own), own), :] = fin_in[...]
    pending.append(last)
    for copy in pending:
        copy.wait_send()


def body(n_fs, *args):
    (tokens, norm_gain, w_query, w_key, w_value, w_gate, mixer_gain, w_out, channel_gain,
     w_left, w_right, taps_left, taps_right, w_down) = args
    groups = w_query.shape[1] // DK
    if (
        groups < 2
        or n_fs % groups
        or n_fs == groups
        or lax.axis_size("tp") != 2
        or tokens.shape[0] != BLOCK
        or (w_left.shape[1] // groups) % 128
        or w_left.shape[1] % groups
        or w_out.shape[1] % 128
        or w_query.shape[0] % 16
    ):
        return plain_body(*args)
    length, width = tokens.shape
    heads = groups * lax.axis_size("tp")
    cq, cv, cf = w_query.shape[1] // groups, w_value.shape[1] // groups, w_left.shape[1] // groups
    planes = n_fs // groups
    own = length // 2
    cos_t, sin_t = turning(length, DK)
    vmem = pl.BlockSpec(memory_space=pltpu.VMEM)
    bf, f32, dma = jnp.bfloat16, jnp.float32, pltpu.SemaphoreType.DMA
    return pl.pallas_call(
        functools.partial(layer_kernel, n_fs, groups),
        out_shape=jax.ShapeDtypeStruct(tokens.shape, bf),
        in_specs=[vmem] * 17,
        out_specs=vmem,
        scratch_shapes=[
            pltpu.VMEM((width, 2 * cq + 2 * cv), bf),
            pltpu.VMEM((cv, width), bf),
            pltpu.VMEM((width, 2 * cf), bf),
            pltpu.VMEM((cf, width), bf),
            pltpu.VMEM((groups * length, width), bf),
            pltpu.VMEM((groups * length, width), bf),
            pltpu.VMEM((groups * length, 2 * cq + 2 * cv), bf),
            pltpu.VMEM((groups * length, cv), bf),
            pltpu.VMEM((groups * length, cf), bf),
            pltpu.VMEM((2, groups, own, width), bf),
            pltpu.VMEM((2, groups, own, width), bf),
            pltpu.VMEM((groups, own, width), bf),
            pltpu.VMEM((groups, own, width), bf),
            pltpu.VMEM((groups, own, width), bf),
            pltpu.VMEM((groups, own, width), bf),
            pltpu.VMEM((groups, own, width), bf),
            pltpu.VMEM((groups, own, width), bf),
            pltpu.VMEM((own, width), f32),
            pltpu.VMEM((own, width), bf),
            pltpu.VMEM((own, width), bf),
            dma((8, groups)),
            dma((8, groups)),
            dma((8,)),
            dma((4, groups, planes)),
            dma((4, groups, planes)),
            dma((2, groups)),
            dma((2, groups)),
            dma((2, groups)),
            dma((2, groups)),
            dma((2, groups)),
            dma((2, groups)),
            dma((2, groups)),
            dma((2, groups)),
            dma,
            dma,
        ],
        compiler_params=pltpu.CompilerParams(
            collective_id=0, has_side_effects=True, vmem_limit_bytes=60 * 1024 * 1024
        ),
    )(
        tokens, norm_gain[None], w_query, w_key, w_value, w_gate, mixer_gain[None], w_out,
        channel_gain[None], w_left, w_right, taps_left, taps_right, w_down,
        cos_t, sin_t, log_gammas(heads),
    )


def solution(mesh):
    placed = (
        P("fs", None),
        P(),
        P("fs", "tp"),
        P("fs", "tp"),
        P("fs", "tp"),
        P("fs", "tp"),
        P("tp"),
        P("tp", "fs"),
        P(),
        P("fs", "tp"),
        P("fs", "tp"),
        P(None, "tp"),
        P(None, "tp"),
        P("tp", "fs"),
    )
    return jax.shard_map(
        functools.partial(body, mesh.shape["fs"]), mesh=mesh, in_specs=placed, out_specs=P("fs", None), check_vma=False)
```

```python
import functools

import jax
import jax.numpy as jnp
import numpy as np
from jax import lax
from jax.experimental import pallas as pl
from jax.experimental.pallas import tpu as pltpu
from jax.sharding import PartitionSpec as P

DK = 128
DV = 256
BLOCK = 128
MESH = pl.DeviceIdType.MESH


highest = lax.Precision.HIGHEST


def scale_rows(rows_in, gain_vec):
    floats = rows_in.astype(jnp.float32)
    factor = lax.rsqrt(jnp.mean(floats * floats, axis=-1, keepdims=True) + 1e-06)
    return (floats * factor * gain_vec).astype(jnp.bfloat16)


def decays(first_head, count):
    head_ids = first_head + jnp.arange(count, dtype=jnp.float32)
    return jnp.log(1.0 - 2.0 ** (-5.0 - head_ids))


def rotate(heads_in, positions):
    width = heads_in.shape[-1]
    half = width // 2
    freqs = 10000.0 ** (-jnp.arange(half, dtype=jnp.float32) / half)
    angles = positions[:, None] * freqs[None, :]
    cosine = jnp.cos(angles)
    sine = jnp.sin(angles)
    first_half = heads_in[..., :half]
    second_half = heads_in[..., half:]
    return jnp.concatenate(
        [first_half * cosine - second_half * sine, first_half * sine + second_half * cosine],
        axis=-1,
    )


def retention(queries, keys_in, values_in, log_gamma):
    head_count, length, key_width = queries.shape
    value_width = values_in.shape[-1]
    blocks = length // BLOCK
    queries = queries.reshape(head_count, blocks, BLOCK, key_width)
    keys_in = keys_in.reshape(head_count, blocks, BLOCK, key_width)
    values_in = values_in.reshape(head_count, blocks, BLOCK, value_width)
    offsets = jnp.arange(BLOCK, dtype=jnp.float32)
    distance = offsets[:, None] - offsets[None, :]
    weights = jnp.where(
        distance >= 0, jnp.exp(log_gamma[:, None, None] * jnp.maximum(distance, 0.0)), 0.0
    )
    scores = jnp.einsum("hbnd,hbmd->hbnm", queries, keys_in, precision=highest) * weights[:, None]
    inner = jnp.einsum("hbnm,hbme->hbne", scores, values_in, precision=highest)
    key_weight = jnp.exp(log_gamma[:, None] * (BLOCK - 1 - offsets)[None, :])
    contrib = jnp.einsum(
        "hbjd,hbje->hbde", keys_in * key_weight[:, None, :, None], values_in, precision=highest
    )
    block_decay = jnp.exp(log_gamma * BLOCK)[:, None, None]

    def advance(state, contrib_block):
        return (state * block_decay + contrib_block, state)

    _, states = lax.scan(
        advance,
        jnp.zeros((head_count, key_width, value_width), jnp.float32),
        jnp.moveaxis(contrib, 1, 0),
    )
    states = jnp.moveaxis(states, 0, 1)
    query_weight = jnp.exp(log_gamma[:, None] * (offsets + 1.0)[None, :])
    carried = (
        jnp.einsum("hbnd,hbde->hbne", queries, states, precision=highest)
        * query_weight[:, None, :, None]
    )
    return (inner + carried).reshape(head_count, length, value_width)


def head_norm(retained):
    return retained * lax.rsqrt(jnp.mean(retained * retained, axis=-1, keepdims=True) + 1e-06)


def causal_taps(values_in, taps):
    length = values_in.shape[-2]
    padded = jnp.pad(values_in.astype(jnp.float32), ((taps.shape[0] - 1, 0), (0, 0)))
    result = padded[0:length] * taps[0]
    for tap_index in range(1, taps.shape[0]):
        result = result + padded[tap_index : tap_index + length] * taps[tap_index]
    return result


def fold_single(source, weight_piece):
    return jnp.dot(source, weight_piece, preferred_element_type=jnp.float32)


def collect_single(source, weight):
    return fold_single(source, lax.all_gather(weight, "fs", axis=0, tiled=True))


def plain_body(
    tokens,
    norm_gain,
    w_query,
    w_key,
    w_value,
    w_gate,
    mixer_gain,
    w_out,
    channel_gain,
    w_left,
    w_right,
    taps_left,
    taps_right,
    w_down,
):
    length = tokens.shape[0]
    normed = scale_rows(tokens, norm_gain)
    queries = collect_single(normed, w_query)
    keys_proj = collect_single(normed, w_key)
    values_proj = collect_single(normed, w_value)
    gates = collect_single(normed, w_gate)
    queries = queries.astype(jnp.bfloat16)
    keys_proj = keys_proj.astype(jnp.bfloat16)
    values_proj = values_proj.astype(jnp.bfloat16)
    gates = gates.astype(jnp.bfloat16)
    heads_here = w_query.shape[1] // DK
    first_head = (lax.axis_index("tp") * heads_here).astype(jnp.float32)
    log_gamma = decays(first_head, heads_here)
    positions = jnp.arange(length, dtype=jnp.float32)

    def split_heads(rows_in, width):
        return rows_in.astype(jnp.float32).reshape(length, heads_here, width).transpose(1, 0, 2)

    retained = head_norm(
        retention(
            rotate(split_heads(queries, DK), positions),
            rotate(split_heads(keys_proj, DK), positions),
            split_heads(values_proj, DV),
            log_gamma,
        )
    )
    retained = retained.transpose(1, 0, 2).reshape(length, heads_here * DV)
    hidden = (retained * mixer_gain * jax.nn.silu(gates.astype(jnp.float32))).astype(jnp.bfloat16)
    rows_own = length // lax.axis_size("tp")
    first_row = lax.axis_index("tp") * rows_own
    out_whole = lax.all_gather(w_out, "fs", axis=1, tiled=True)
    mixer_total = lax.psum_scatter(
        jnp.dot(hidden, out_whole, preferred_element_type=jnp.float32).astype(jnp.bfloat16),
        "tp",
        scatter_dimension=0,
        tiled=True,
    ).astype(jnp.float32)
    residual = lax.dynamic_slice_in_dim(tokens, first_row, rows_own, 0)
    middle_own = (residual.astype(jnp.float32) + mixer_total).astype(jnp.bfloat16)
    middle = lax.all_gather(middle_own, "tp", axis=0, tiled=True)
    normed_mid = scale_rows(middle, channel_gain)
    left = collect_single(normed_mid, w_left)
    right = collect_single(normed_mid, w_right)
    left = left.astype(jnp.bfloat16)
    right = right.astype(jnp.bfloat16)
    gated = (jax.nn.silu(causal_taps(left, taps_left)) * causal_taps(right, taps_right)).astype(
        jnp.bfloat16
    )
    down_whole = lax.all_gather(w_down, "fs", axis=1, tiled=True)
    channel_part = jnp.dot(gated, down_whole, preferred_element_type=jnp.float32)
    channel_total = lax.psum(channel_part.astype(jnp.bfloat16), "tp").astype(jnp.float32)
    return (middle.astype(jnp.float32) + channel_total).astype(jnp.bfloat16)


def log_gammas(head_count):
    table = np.log(1.0 - 2.0 ** (-5.0 - np.arange(head_count, dtype=np.float64)))
    return np.repeat(table[:, None], BLOCK, axis=1).astype(np.float32)


def turning(length, width):
    half = width // 2
    freqs = np.float32(10000.0) ** (-np.arange(half, dtype=np.float32) / np.float32(half))
    angles = (np.arange(length, dtype=np.float32)[:, None] * freqs[None, :]).astype(np.float64)
    cosine, sine = np.cos(angles), np.sin(angles)
    return (
        np.concatenate([cosine, cosine], axis=1).astype(np.float32),
        np.concatenate([-sine, sine], axis=1).astype(np.float32),
    )


def silu(v):
    return v / (1.0 + jnp.exp(-v))


def normed_rows(floats, gain):
    factor = lax.rsqrt(jnp.mean(floats * floats, axis=-1, keepdims=True) + 1e-06)
    return (floats * factor * gain).astype(jnp.bfloat16)


def layer_kernel(
    n_fs,
    groups,
    tokens,
    norm_gain,
    wq,
    wk,
    wv,
    wg,
    mixer_gain,
    wo,
    channel_gain,
    wl,
    wr,
    taps_left,
    taps_right,
    wd,
    cos_t,
    sin_t,
    gammas,
    out,
    w1,
    wout,
    wlr,
    wdown,
    nt,
    nm,
    qkvg,
    hid,
    gated,
    part1,
    part2,
    xb1,
    xb2,
    sb1,
    sb2,
    rb1,
    rb2,
    mid,
    acc,
    both,
    fin,
    fin_in,
    s1_send,
    s1_recv,
    self_sem,
    s2_send,
    s2_recv,
    a_send,
    a_recv,
    f_send,
    f_recv,
    x_send,
    x_recv,
    r_send,
    r_recv,
    o_send,
    o_recv,
):
    fs, tp = lax.axis_index("fs"), lax.axis_index("tp")
    planes = n_fs // groups
    z, q = fs // planes, lax.rem(fs, planes)
    other = 1 - tp
    length, width = tokens.shape
    own = length // 2
    few = own // 2
    later = range(1, groups)
    everyone = range(groups)
    kb = wq.shape[0]
    nb = wo.shape[1]
    cq, cv, cf = wq.shape[1] // groups, wv.shape[1] // groups, wl.shape[1] // groups

    def zpeer(step):
        return lax.rem(z + step, groups)

    def zback(step):
        return lax.rem(z + groups - step, groups)

    def zdev(target):
        return {"fs": target * planes + q, "tp": tp}

    partner = {"fs": fs, "tp": other}

    def lanes(index, size):
        return pl.ds(pl.multiple_of(index * size, 128), size)

    def rows(index, size):
        return pl.ds(pl.multiple_of(index * size, size), size)

    def region(cls, f):
        if cls == 0:
            return w1.at[rows(f, kb), :]
        if cls == 1:
            return wout.at[:, lanes(f, nb)]
        if cls == 2:
            return wlr.at[rows(f, kb), :]
        return wdown.at[:, lanes(f, nb)]

    pieces = (
        (0, lambda c: wq.at[:, lanes(c, cq)], lambda f: w1.at[rows(f, kb), pl.ds(0, cq)]),
        (0, lambda c: wk.at[:, lanes(c, cq)], lambda f: w1.at[rows(f, kb), pl.ds(cq, cq)]),
        (0, lambda c: wv.at[:, lanes(c, cv)], lambda f: w1.at[rows(f, kb), pl.ds(2 * cq, cv)]),
        (0, lambda c: wg.at[:, lanes(c, cv)], lambda f: w1.at[rows(f, kb), pl.ds(2 * cq + cv, cv)]),
        (1, lambda c: wo.at[rows(c, cv), :], lambda f: wout.at[:, lanes(f, nb)]),
        (2, lambda c: wl.at[:, lanes(c, cf)], lambda f: wlr.at[rows(f, kb), pl.ds(0, cf)]),
        (2, lambda c: wr.at[:, lanes(c, cf)], lambda f: wlr.at[rows(f, kb), pl.ds(cf, cf)]),
        (3, lambda c: wd.at[rows(c, cf), :], lambda f: wdown.at[:, lanes(f, nb)]),
    )

    barrier = pltpu.get_barrier_semaphore()
    for step in range(1, groups):
        pl.semaphore_signal(barrier, inc=1, device_id=zdev(zpeer(step)), device_id_type=MESH)
    qx = q + 1 - 2 * lax.rem(q, 2)
    qy = q + 2 - 4 * (q // 2)
    to_x = {"fs": z * planes + qx, "tp": tp}
    to_y = {"fs": z * planes + qy, "tp": tp}
    for device in (to_x, to_y):
        pl.semaphore_signal(barrier, inc=1, device_id=device, device_id_type=MESH)
    pl.semaphore_signal(barrier, inc=1, device_id=partner, device_id_type=MESH)

    keeps = []
    for i, (cls, src, dst) in enumerate(pieces):
        keep = pltpu.make_async_copy(src(z), dst(fs), self_sem.at[i])
        keep.start()
        keeps.append(keep)

    def own_rows(seq, half):
        return pl.ds(pl.multiple_of(seq * length + half * own, own), own)

    my_half = pl.ds(pl.multiple_of(tp * own, own), own)
    nt[own_rows(z, tp), :] = normed_rows(tokens[my_half, :].astype(jnp.float32), norm_gain[...])
    pl.semaphore_wait(barrier, groups - 1 + 2 + 1)

    def remote(src, dst, ssem, rsem, device):
        return pltpu.make_async_remote_copy(
            src_ref=src, dst_ref=dst, send_sem=ssem, recv_sem=rsem,
            device_id=device, device_id_type=MESH,
        )

    pending = []

    def go(copy):
        copy.start()
        pending.append(copy)

    def spread(buf, which, place):
        mine = buf.at[place(z, tp), :]
        for step in later:
            go(remote(mine, mine, a_send.at[which, step], a_recv.at[which, step], zdev(zpeer(step))))
        go(remote(mine, mine, f_send.at[which, 0], f_recv.at[which, 0], partner))

    def pass_on(buf, which, place):
        for step in later:
            got = buf.at[place(zback(step), tp), :]
            remote(got, got, a_send.at[which, step], a_recv.at[which, step], zdev(zpeer(step))).wait_recv()
            go(remote(got, got, f_send.at[which, step], f_recv.at[which, step], partner))

    def await_pass(buf, which, place):
        for step in everyone:
            got = buf.at[place(zback(step), other), :]
            remote(got, got, f_send.at[which, step], f_recv.at[which, step], partner).wait_recv()

    def in_half(half):
        def place(seq, core):
            return pl.ds(pl.multiple_of(half * groups * own + seq * own + core * few, few), few)
        return place

    def first_leg(cls):
        for step in range(1, groups):
            for i, (c, src, dst) in enumerate(pieces):
                if c == cls:
                    target = zpeer(step)
                    go(remote(src(target), dst(fs), s1_send.at[i, step], s1_recv.at[i, step], zdev(target)))

    def half_of(cls, f, half):
        block = region(cls, f)
        size = (kb, cv, kb, cf)[cls] // 2
        return block.at[pl.ds(half * size, size), :]

    hops = ((0, to_x), (1, to_y), (1, to_x), (0, to_y))

    def hop_copy(cls, step, from_q, half, slot, device):
        ref = half_of(cls, zback(step) * planes + from_q, half)
        return remote(ref, ref, s2_send.at[cls, step, slot], s2_recv.at[cls, step, slot], device)

    def direct(cls, step):
        f = zback(step) * planes + q
        for i, (c, src, dst) in enumerate(pieces):
            if c == cls:
                if step == 0:
                    keeps[i].wait()
                else:
                    remote(src(z), dst(f), s1_send.at[i, step], s1_recv.at[i, step], zdev(zpeer(step))).wait_recv()
        for slot, (half, device) in enumerate(hops):
            go(hop_copy(cls, step, q, half, slot, device))

    def relay(cls, step):
        hop_copy(cls, step, qx, 0, 0, to_x).wait_recv()
        go(hop_copy(cls, step, qx, 0, 4, to_y))
        hop_copy(cls, step, qy, 1, 1, to_y).wait_recv()
        go(hop_copy(cls, step, qy, 1, 5, to_x))

    def await_leg(cls):
        diagonal = planes - 1 - q
        for step in range(groups):
            hop_copy(cls, step, qx, 1, 2, to_x).wait_recv()
            hop_copy(cls, step, qy, 0, 3, to_y).wait_recv()
            hop_copy(cls, step, diagonal, 0, 4, to_y).wait_recv()
            hop_copy(cls, step, diagonal, 1, 5, to_x).wait_recv()

    first_leg(0)
    spread(nt, 0, own_rows)
    first_leg(1)
    first_leg(2)
    first_leg(3)
    direct(0, 0)
    direct(2, 0)
    relay(0, 0)
    for step in later:
        direct(0, step)
    for step in later:
        relay(0, step)
    direct(1, 0)
    pass_on(nt, 0, own_rows)
    await_pass(nt, 0, own_rows)
    await_leg(0)

    head = tp * groups + z
    log_gamma = gammas[pl.ds(head, 1), :]
    distance = (
        lax.broadcasted_iota(jnp.int32, (length, length), 0)
        - lax.broadcasted_iota(jnp.int32, (length, length), 1)
    ).astype(jnp.float32)
    decay = jnp.where(distance >= 0, jnp.exp(log_gamma * jnp.maximum(distance, 0.0)), 0.0)
    chunk = 2 * length if (groups % 2 == 0) else length

    @pl.loop(0, groups * length // chunk)
    def _(at):
        span = rows(at, chunk)
        qkvg[span, :] = jnp.dot(
            nt[span, :], w1[...], preferred_element_type=jnp.float32
        ).astype(jnp.bfloat16)

    for step in later:
        direct(1, step)
    relay(2, 0)
    direct(3, 0)

    @pl.loop(0, groups)
    def _(at):
        span = rows(at, length)
        block = qkvg[span, :].astype(jnp.float32)

        def turn(x):
            return x * cos_t[...] + pltpu.roll(x, cq // 2, 1) * sin_t[...]

        rq = turn(block[:, :cq])
        rk = turn(block[:, cq : 2 * cq])
        scores = lax.dot_general(
            rq, rk, (((1,), (1,)), ((), ())), precision=highest, preferred_element_type=jnp.float32
        ) * decay
        kept = jnp.dot(
            scores, block[:, 2 * cq : 2 * cq + cv], precision=highest,
            preferred_element_type=jnp.float32,
        )
        kept = kept * lax.rsqrt(jnp.mean(kept * kept, axis=-1, keepdims=True) + 1e-06)
        gain = mixer_gain[:, lanes(z, cv)]
        whole = (kept * gain * silu(block[:, 2 * cq + cv :])).astype(jnp.bfloat16)
        hid[rows(at, own), :] = whole[:own]
        hid[rows(at + groups, own), :] = whole[own:]

    def multiply(left, weight, part, xb, which, half):
        value = jnp.dot(
            left[rows(half, groups * own), :], weight[...], preferred_element_type=jnp.float32
        ).astype(jnp.bfloat16)
        for g in everyone:
            part[half, 0, g] = value[g * own : g * own + few]
            part[half, 1, g] = value[g * own + few : (g + 1) * own]
        go(remote(part.at[half, other], xb.at[half], x_send.at[which, half], x_recv.at[which, half], partner))

    def reduce_pair(part, xb, sb, rb, acc, which, half):
        remote(part.at[half, other], xb.at[half], x_send.at[which, half], x_recv.at[which, half], partner).wait_recv()

        def pair(g):
            return part[half, tp, g].astype(jnp.float32) + xb[half, g].astype(jnp.float32)

        for step in later:
            sb[half, step] = pair(zpeer(step)).astype(jnp.bfloat16)
            go(remote(sb.at[half, step], rb.at[half, step], r_send.at[which, half, step],
                      r_recv.at[which, half, step], zdev(zpeer(step))))
        acc[half] = pair(z)

    def collect(sb, rb, acc, which, half):
        value = acc[half]
        for step in later:
            remote(sb.at[half, step], rb.at[half, step], r_send.at[which, half, step],
                   r_recv.at[which, half, step], zdev(zpeer(step))).wait_recv()
            value = value + rb[half, step].astype(jnp.float32)
        return value

    def natural(half, core):
        return pl.ds(pl.multiple_of(half * own + core * few, few), few)

    for step in everyone:
        relay(1, step)
    await_leg(1)
    multiply(hid, wout, part1, xb1, 0, 0)
    multiply(hid, wout, part1, xb1, 0, 1)
    reduce_pair(part1, xb1, sb1, rb1, acc, 0, 0)
    reduce_pair(part1, xb1, sb1, rb1, acc, 0, 1)
    for step in later:
        direct(2, step)
    for step in later:
        relay(2, step)
    for half in range(2):
        middle = (
            tokens[natural(half, tp), :].astype(jnp.float32) + collect(sb1, rb1, acc, 0, half)
        ).astype(jnp.bfloat16).astype(jnp.float32)
        mid[half] = middle
        nm[in_half(half)(z, tp), :] = normed_rows(middle, channel_gain[...])
        spread(nm, 1 + half, in_half(half))
    for step in later:
        direct(3, step)
    for step in everyone:
        relay(3, step)

    place = lax.rem(lax.broadcasted_iota(jnp.int32, (groups * own, 1), 0), own)

    def convolve(half, low, taps):
        x = both[half, :, low : low + cf].astype(jnp.float32)
        count = taps.shape[0]
        weights = taps[:, lanes(z, cf)]
        result = x * weights[count - 1 :, :]
        for back in range(1, count):
            if half:
                before = both[0, :, low : low + cf].astype(jnp.float32)
                before = pltpu.roll(before, back + (groups - 1) * own, 0)
            else:
                before = 0.0
            moved = jnp.where(place >= back, pltpu.roll(x, back, 0), before)
            result = result + moved * weights[count - 1 - back : count - back, :]
        return result

    for half in range(2):
        pass_on(nm, 1 + half, in_half(half))
        await_pass(nm, 1 + half, in_half(half))
        if not half:
            await_leg(2)
        both[half] = jnp.dot(
            nm[rows(half, groups * own), :], wlr[...], preferred_element_type=jnp.float32
        ).astype(jnp.bfloat16)
        gated[rows(half, groups * own), :] = (
            silu(convolve(half, 0, taps_left)) * convolve(half, cf, taps_right)
        ).astype(jnp.bfloat16)
        if not half:
            await_leg(3)
        multiply(gated, wdown, part2, xb2, 1, half)
        reduce_pair(part2, xb2, sb2, rb2, acc, 1, half)
    for half in range(2):
        mine = natural(half, tp)
        value = (mid[half] + collect(sb2, rb2, acc, 1, half)).astype(jnp.bfloat16)
        fin[half] = value
        go(remote(fin.at[half], fin_in.at[half], o_send.at[half], o_recv.at[half], partner))
        out[mine, :] = value
    for half in range(2):
        remote(fin.at[half], fin_in.at[half], o_send.at[half], o_recv.at[half], partner).wait_recv()
        out[natural(half, other), :] = fin_in[half]
    for copy in pending:
        copy.wait_send()


def body(n_fs, *args):
    (tokens, norm_gain, w_query, w_key, w_value, w_gate, mixer_gain, w_out, channel_gain,
     w_left, w_right, taps_left, taps_right, w_down) = args
    groups = w_query.shape[1] // DK
    if (
        groups < 2
        or n_fs % groups
        or n_fs != 4 * groups
        or lax.axis_size("tp") != 2
        or tokens.shape[0] != BLOCK
        or (w_left.shape[1] // groups) % 128
        or w_left.shape[1] % groups
        or w_out.shape[1] % 128
        or w_query.shape[0] % 16
    ):
        return plain_body(*args)
    length, width = tokens.shape
    heads = groups * lax.axis_size("tp")
    cq, cv, cf = w_query.shape[1] // groups, w_value.shape[1] // groups, w_left.shape[1] // groups
    planes = n_fs // groups
    own = length // 2
    few = own // 2
    cos_t, sin_t = turning(length, DK)
    vmem = pl.BlockSpec(memory_space=pltpu.VMEM)
    held = pl.BlockSpec(memory_space=pl.ANY)
    bf, f32, dma = jnp.bfloat16, jnp.float32, pltpu.SemaphoreType.DMA
    return pl.pallas_call(
        functools.partial(layer_kernel, n_fs, groups),
        out_shape=jax.ShapeDtypeStruct(tokens.shape, bf),
        in_specs=[vmem] * 2 + [held] * 4 + [vmem, held, vmem] + [held] * 2 + [vmem] * 2 + [held] + [vmem] * 3,
        out_specs=vmem,
        scratch_shapes=[
            pltpu.VMEM((width, 2 * cq + 2 * cv), bf),
            pltpu.VMEM((cv, width), bf),
            pltpu.VMEM((width, 2 * cf), bf),
            pltpu.VMEM((cf, width), bf),
            pltpu.VMEM((groups * length, width), bf),
            pltpu.VMEM((groups * length, width), bf),
            pltpu.VMEM((groups * length, 2 * cq + 2 * cv), bf),
            pltpu.VMEM((groups * length, cv), bf),
            pltpu.VMEM((groups * length, cf), bf),
            pltpu.VMEM((2, 2, groups, few, width), bf),
            pltpu.VMEM((2, 2, groups, few, width), bf),
            pltpu.VMEM((2, groups, few, width), bf),
            pltpu.VMEM((2, groups, few, width), bf),
            pltpu.VMEM((2, groups, few, width), bf),
            pltpu.VMEM((2, groups, few, width), bf),
            pltpu.VMEM((2, groups, few, width), bf),
            pltpu.VMEM((2, groups, few, width), bf),
            pltpu.VMEM((2, few, width), f32),
            pltpu.VMEM((2, few, width), f32),
            pltpu.VMEM((2, groups * own, 2 * cf), bf),
            pltpu.VMEM((2, few, width), bf),
            pltpu.VMEM((2, few, width), bf),
            dma((8, groups)),
            dma((8, groups)),
            dma((8,)),
            dma((4, groups, 6)),
            dma((4, groups, 6)),
            dma((3, groups)),
            dma((3, groups)),
            dma((3, groups)),
            dma((3, groups)),
            dma((2, 2)),
            dma((2, 2)),
            dma((2, 2, groups)),
            dma((2, 2, groups)),
            dma((2,)),
            dma((2,)),
        ],
        compiler_params=pltpu.CompilerParams(
            collective_id=0, has_side_effects=True, vmem_limit_bytes=60 * 1024 * 1024
        ),
    )(
        tokens, norm_gain[None], w_query, w_key, w_value, w_gate, mixer_gain[None], w_out,
        channel_gain[None], w_left, w_right, taps_left, taps_right, w_down,
        cos_t, sin_t, log_gammas(heads),
    )


def solution(mesh):
    placed = (
        P("fs", None),
        P(),
        P("fs", "tp"),
        P("fs", "tp"),
        P("fs", "tp"),
        P("fs", "tp"),
        P("tp"),
        P("tp", "fs"),
        P(),
        P("fs", "tp"),
        P("fs", "tp"),
        P(None, "tp"),
        P(None, "tp"),
        P("tp", "fs"),
    )
    return jax.shard_map(
        functools.partial(body, mesh.shape["fs"]), mesh=mesh, in_specs=placed, out_specs=P("fs", None), check_vma=False)
```
